32 devices in a mesh: dp: 4 (over y, x), kv: 4 (over z), tp: 2 (over core).
Axes of the slice: x: 2, y: 2, z: 4, core: 2. Of those that a mesh axis runs over, the one named last changes fastest.
Arguments:
- tokens: bfloat16 [128, 4096], P('dp', ('kv', 'tp')), parts along dimension 0, may hold values from -12 to 12
- norm_gain: float32 [4096], replicated, may hold values from 0.1 to 1.9
- w_query: bfloat16 [4096, 3072], P(None, ('kv', 'tp')), may hold values from -0.09375 to 0.09375
- w_key: bfloat16 [4096, 3072], P(None, ('kv', 'tp')), may hold values from -0.09375 to 0.09375
- w_value: bfloat16 [4096, 3072], P(None, ('kv', 'tp')), may hold values from -0.09375 to 0.09375
- w_gate: bfloat16 [4096, 3072], P(None, ('kv', 'tp')), may hold values from -0.09375 to 0.09375
- w_output: bfloat16 [3072, 4096], P(None, ('kv', 'tp')), may hold values from -0.109375 to 0.109375
- decay_rate: float32 [24], replicated, may hold values from 0.003 to 2
- state: float32 [32, 24, 128, 128], P(('dp', 'kv', 'tp')), parts along dimension 0, may hold values from -0.54 to 0.54
- prev_keys: bfloat16 [32, 4, 3072], P(('dp', 'kv', 'tp')), parts along dimension 0, may hold values from -0.5390625 to 0.5390625
- prev_values: bfloat16 [32, 4, 3072], P(('dp', 'kv', 'tp')), parts along dimension 0, may hold values from -6 to 6
- accepted: int32 [32], P(('dp', 'kv', 'tp')), parts along dimension 0, may hold values from 0 to 4
- parents: int32 [32, 4], P(('dp', 'kv', 'tp')), parts along dimension 0, may hold values from -1 to 2, as said below
- seq_length: int32 [32], P(('dp', 'kv', 'tp')), parts along dimension 0, may hold values from 1 to 8191
Outputs:
- output: bfloat16 [128, 4096], P('dp', ('kv', 'tp')), parts along dimension 0
- carried: float32 [32, 24, 128, 128], P(('dp', 'kv', 'tp')), parts along dimension 0
The draws below stay inside these ranges and needn't reach their ends.
There are 4 independent parts, one for each index of `dp`. The reference program is written for one: setup_inputs(seed, part) draws one part's arguments, and reference() takes and returns one part's arrays. A program takes and returns all parts, laid end to end along the dimension named above; an argument that names none is the same for every part. Nothing has to cross between parts.
Inputs may be any that keep to these rules, and one draw needn't show every extreme that they name: parents[s, i] is -1 or an earlier proposal of the same sequence; proposal 0 has -1.
All inputs are finite; a program needn't handle non-finite values.
Results may differ from the reference program's by a relative error of at most 0.013.
Values may be sent and summed in bfloat16 or wider, within the bound.
A program may use at most 64 MiB of HBM per device.

```python
import jax
import jax.numpy as jnp
from jax import lax

D = 4096
HEADS = 24
HEAD_DIM = 128
PROPS = 4
HID = 3072
SEQS = 8
TOKENS = 32


def draw_tokens(key, part):
    second = jax.random.fold_in(jax.random.fold_in(key, 11), 1)
    ramp = jnp.arange(D, dtype=jnp.float32) / (D - 1)
    column_scale = jnp.exp(jnp.log(3.0) * ramp) / 1.7
    values = jnp.clip(jax.random.normal(second, (TOKENS, D), jnp.float32), -6.0, 6.0) * column_scale[None, :]
    return values.astype(jnp.bfloat16)


def draw_decay_rate(key, part):
    first, second, third = jax.random.split(jax.random.fold_in(key, 23), 3)
    fast = jax.random.uniform(second, (HEADS,), jnp.float32) < 0.5
    quick = jnp.exp(jax.random.uniform(first, (HEADS,), jnp.float32, jnp.log(0.3), jnp.log(2.0)))
    slow = jnp.exp(jax.random.uniform(third, (HEADS,), jnp.float32, jnp.log(0.01), jnp.log(0.1)))
    rates = jnp.where(fast, quick, slow)
    return rates.astype(jnp.float32)


def draw_parents(key, part):
    limits = jnp.arange(PROPS, dtype=jnp.int32)[None, :]
    upper = jnp.broadcast_to(limits, (SEQS, PROPS))
    return jax.random.randint(jax.random.fold_in(key, 37), (SEQS, PROPS), -1, upper).astype(jnp.int32)


def touch_ends(result, key, least, high):
    spot = [jax.random.randint(jax.random.fold_in(key, axis), (), 0, length) for axis, length in enumerate(result.shape)]
    widest = result.shape.index(max(result.shape))
    beside = spot[:widest] + [(spot[widest] + 1) % result.shape[widest]] + spot[widest + 1:]
    return result.at[tuple(spot)].set(least).at[tuple(beside)].set(high)


def block_levels(own_key, shape, pieces, low, largest):
    gain, own = 1.0, jax.random.fold_in(own_key, 6)
    for axis_at, blocks in pieces:
        heights = jnp.exp(jax.random.uniform(jax.random.fold_in(own, axis_at), (blocks,), jnp.float32, low / len(pieces), largest / len(pieces)))
        gain = gain * jnp.repeat(heights, shape[axis_at] // blocks).reshape([-1 if axis == axis_at else 1 for axis in range(len(shape))])
    return gain


def gaussian(rng, dims, spread, reach, cuts=(), held_as=jnp.bfloat16):
    drawn = spread * jax.random.normal(rng, dims, jnp.float32)
    if cuts:
        drawn = drawn * block_levels(rng, dims, cuts, -0.22, 0.18)
    return jnp.clip(drawn, -reach, reach).astype(held_as)


def setup_inputs(seed: int = 0, part: int = 0) -> dict:
    key_of = jax.random.split(jax.random.key(seed), 15)
    part_splits = jax.random.split(jax.random.fold_in(key_of[14], part), 15)
    tokens = draw_tokens(jax.random.fold_in(jax.random.fold_in(key_of[14], part), 71), part)
    norm_gain = jnp.clip(1.0 + 0.18 * jax.random.normal(key_of[1], (D,), jnp.float32), 0.1, 1.9)
    w_query = gaussian(key_of[2], (D, HID), D ** -0.5, 0.09375, ((1, 8),))
    w_key = gaussian(key_of[3], (D, HID), D ** -0.5, 0.09375, ((1, 8),))
    w_value = gaussian(key_of[4], (D, HID), D ** -0.5, 0.09375, ((1, 8),))
    w_gate = gaussian(key_of[5], (D, HID), D ** -0.5, 0.09375, ((1, 8),))
    w_output = gaussian(key_of[6], (HID, D), HID ** -0.5, 0.109375, ((1, 8),))
    decay_rate = draw_decay_rate(jax.random.fold_in(key_of[14], 71), part)
    state = gaussian(part_splits[8], (SEQS, HEADS, HEAD_DIM, HEAD_DIM), 0.09, 0.54, ((0, 8),), jnp.float32)
    prev_keys = gaussian(part_splits[9], (SEQS, PROPS, HID), 0.09, 0.5390625, ((0, 8),))
    prev_values = gaussian(part_splits[10], (SEQS, PROPS, HID), 1.0, 6.0, ((0, 8),))
    accepted = touch_ends(jax.random.randint(part_splits[11], (SEQS,), 0, PROPS + 1), jax.random.fold_in(part_splits[11], 1), 0, PROPS).astype(jnp.int32)
    parents = draw_parents(jax.random.fold_in(jax.random.fold_in(key_of[14], part), 71), part)
    seq_length = touch_ends(jax.random.randint(part_splits[13], (SEQS,), 1, 8192), jax.random.fold_in(part_splits[13], 1), 1, 8191).astype(jnp.int32)
    return dict(tokens=tokens, norm_gain=norm_gain, w_query=w_query, w_key=w_key, w_value=w_value, w_gate=w_gate, w_output=w_output, decay_rate=decay_rate, state=state, prev_keys=prev_keys, prev_values=prev_values, accepted=accepted, parents=parents, seq_length=seq_length)


EPS = 1e-06
HIGH = lax.Precision.HIGHEST

def rotate(tensor, positions):
    half_dim = tensor.shape[-1] // 2
    frequency = 10000.0 ** (-jnp.arange(half_dim, dtype=jnp.float32) / half_dim)
    angles = positions[:, :, None] * frequency[None, None, :]
    cosine = jnp.cos(angles)[:, :, None, :]
    sine_part = jnp.sin(angles)[:, :, None, :]
    first = tensor[..., :half_dim]
    second = tensor[..., half_dim:]
    return jnp.concatenate([first * cosine - second * sine_part, second * cosine + first * sine_part], axis=-1)

def ancestry_of(parents):
    props = parents.shape[1]
    linked = (parents[:, :, None] == jnp.arange(props, dtype=jnp.int32)[None, None, :]).astype(jnp.float32)
    identity = jnp.broadcast_to(jnp.eye(props, dtype=jnp.float32), linked.shape)
    ancestry = identity
    power = identity
    for hop in range(props - 1):
        power = jnp.einsum('bij,bjk->bik', power, linked, precision=HIGH)
        ancestry = ancestry + power
    depths = lax.optimization_barrier(jnp.sum(ancestry, axis=-1)) - 1.0
    return (ancestry, depths)

def advance(state, prev_keys, prev_values, accepted, decays):
    nseq, props, width = prev_keys.shape
    heads = decays.shape[0]
    head_dim = width // heads
    old_keys = prev_keys.astype(jnp.float32).reshape(nseq, props, heads, head_dim)
    old_values = prev_values.astype(jnp.float32).reshape(nseq, props, heads, head_dim)
    steps_done = accepted.astype(jnp.float32)[:, None]
    index = jnp.arange(props, dtype=jnp.float32)[None, :]
    age = jnp.maximum(steps_done - 1.0 - index, 0.0)
    weights = jnp.where((index < steps_done)[:, :, None], jnp.exp(-decays[None, None, :] * age[:, :, None]), 0.0)
    kept = jnp.exp(-decays[None, :] * steps_done)
    added = jnp.einsum('bphd,bphe->bhde', old_keys * weights[..., None], old_values, precision=HIGH)
    return kept[:, :, None, None] * state + added

def retain(queries, key_rows, val_rows, gate_rows, decays, carried, parents, accepted, seq_length):
    nseq, props, heads, head_dim = queries.shape
    ancestry, depths = ancestry_of(parents)
    positions = (seq_length + accepted).astype(jnp.float32)[:, None] + depths
    rotated_q = rotate(queries.astype(jnp.float32), positions)
    rotated_k = rotate(key_rows.astype(jnp.float32), positions) * head_dim ** (-0.5)
    scores = jnp.einsum('bihd,bjhd->bhij', rotated_q, rotated_k, precision=HIGH)
    spacing = jnp.maximum(depths[:, :, None] - depths[:, None, :], 0.0)
    weighting = ancestry[:, None] * jnp.exp(-decays[None, :, None, None] * spacing[:, None])
    within = jnp.einsum('bhij,bjhe->bihe', scores * weighting, val_rows.astype(jnp.float32), precision=HIGH)
    state_scale = jnp.exp(-decays[None, None, :] * (depths[:, :, None] + 1.0))
    from_state = jnp.einsum('bihd,bhde->bihe', rotated_q, carried, precision=HIGH) * state_scale[..., None]
    mixed_raw = within + from_state
    average = lax.optimization_barrier(jnp.mean(mixed_raw, axis=-1, keepdims=True))
    centred = mixed_raw - average
    variance = lax.optimization_barrier(jnp.mean(centred * centred, axis=-1, keepdims=True))
    normed = (centred * lax.rsqrt(variance + EPS)).reshape(nseq * props, heads * head_dim)
    gates = gate_rows.astype(jnp.float32).reshape(nseq * props, heads * head_dim)
    return (normed * jax.nn.silu(gates)).astype(jnp.bfloat16)

def reference(tokens, norm_gain, w_query, w_key, w_value, w_gate, w_output, decay_rate, state, prev_keys, prev_values, accepted, parents, seq_length):
    feats = tokens.astype(jnp.float32)
    scale = lax.rsqrt(lax.optimization_barrier(jnp.mean(feats * feats, axis=-1, keepdims=True)) + EPS)
    normed = (feats * scale * norm_gain[None, :]).astype(jnp.bfloat16)
    nseq = state.shape[0]
    heads = decay_rate.shape[0]
    head_dim = state.shape[2]
    props = parents.shape[1]

    def project(weight):
        rows = jnp.dot(normed, weight, preferred_element_type=jnp.float32).astype(jnp.bfloat16)
        return rows.reshape(nseq, props, heads, head_dim)
    carried = advance(state, prev_keys, prev_values, accepted, decay_rate)
    mixed = retain(project(w_query), project(w_key), project(w_value), project(w_gate), decay_rate, carried, parents, accepted, seq_length)
    output = jnp.dot(mixed, w_output, preferred_element_type=jnp.float32).astype(jnp.bfloat16)
    return (output, carried)
```

```python
import functools

import jax
import jax.numpy as jnp
import numpy as np
from jax import lax
from jax.experimental import pallas as pl
from jax.experimental.pallas import tpu as pltpu
from jax.sharding import PartitionSpec as P

EPS = 1e-06
HIGH = lax.Precision.HIGHEST


def rotate(tensor, positions):
    half_dim = tensor.shape[-1] // 2
    frequency = 10000.0 ** (-jnp.arange(half_dim, dtype=jnp.float32) / half_dim)
    angles = positions[:, :, None] * frequency[None, None, :]
    cosine = jnp.cos(angles)[:, :, None, :]
    sine_part = jnp.sin(angles)[:, :, None, :]
    first = tensor[..., :half_dim]
    second = tensor[..., half_dim:]
    return jnp.concatenate(
        [first * cosine - second * sine_part, second * cosine + first * sine_part], axis=-1
    )


def ancestry_of(parents):
    props = parents.shape[1]
    linked = (parents[:, :, None] == jnp.arange(props, dtype=jnp.int32)[None, None, :]).astype(
        jnp.float32
    )
    identity = jnp.broadcast_to(jnp.eye(props, dtype=jnp.float32), linked.shape)
    ancestry = identity
    power = identity
    for hop in range(props - 1):
        power = jnp.einsum("bij,bjk->bik", power, linked, precision=HIGH)
        ancestry = ancestry + power
    depths = jnp.sum(ancestry, axis=-1) - 1.0
    return (ancestry, depths)


def advance(state, prev_keys, prev_values, accepted, decays):
    nseq, props, width = prev_keys.shape
    heads = decays.shape[0]
    head_dim = width // heads
    old_keys = prev_keys.astype(jnp.float32).reshape(nseq, props, heads, head_dim)
    old_values = prev_values.astype(jnp.float32).reshape(nseq, props, heads, head_dim)
    steps_done = accepted.astype(jnp.float32)[:, None]
    index = jnp.arange(props, dtype=jnp.float32)[None, :]
    age = jnp.maximum(steps_done - 1.0 - index, 0.0)
    weights = jnp.where(
        (index < steps_done)[:, :, None], jnp.exp(-decays[None, None, :] * age[:, :, None]), 0.0
    )
    kept = jnp.exp(-decays[None, :] * steps_done)
    added = jnp.einsum("bphd,bphe->bhde", old_keys * weights[..., None], old_values, precision=HIGH)
    return kept[:, :, None, None] * state + added


def retain(queries, key_rows, val_rows, gate_rows, decays, carried, parents, accepted, seq_length):
    nseq, props, heads, head_dim = queries.shape
    ancestry, depths = ancestry_of(parents)
    positions = (seq_length + accepted).astype(jnp.float32)[:, None] + depths
    rotated_q = rotate(queries.astype(jnp.float32), positions)
    rotated_k = rotate(key_rows.astype(jnp.float32), positions) * head_dim ** (-0.5)
    scores = jnp.einsum("bihd,bjhd->bhij", rotated_q, rotated_k, precision=HIGH)
    spacing = jnp.maximum(depths[:, :, None] - depths[:, None, :], 0.0)
    weighting = ancestry[:, None] * jnp.exp(-decays[None, :, None, None] * spacing[:, None])
    within = jnp.einsum(
        "bhij,bjhe->bihe", scores * weighting, val_rows.astype(jnp.float32), precision=HIGH
    )
    state_scale = jnp.exp(-decays[None, None, :] * (depths[:, :, None] + 1.0))
    from_state = (
        jnp.einsum("bihd,bhde->bihe", rotated_q, carried, precision=HIGH) * state_scale[..., None]
    )
    mixed_raw = within + from_state
    average = jnp.mean(mixed_raw, axis=-1, keepdims=True)
    centred = mixed_raw - average
    variance = jnp.mean(centred * centred, axis=-1, keepdims=True)
    normed = (centred * lax.rsqrt(variance + EPS)).reshape(nseq * props, heads * head_dim)
    gates = gate_rows.astype(jnp.float32).reshape(nseq * props, heads * head_dim)
    return (normed * jax.nn.silu(gates)).astype(jnp.bfloat16)


def per_device(
    tokens,
    norm_gain,
    w_query,
    w_key,
    w_value,
    w_gate,
    w_output,
    decay_rate,
    state,
    prev_keys,
    prev_values,
    accepted,
    parents,
    seq_length,
):
    weights = jnp.concatenate([w_query, w_key, w_value, w_gate], axis=1)
    columns = weights.shape[1]
    whole = lax.all_gather(tokens, ("kv", "tp"), axis=1, tiled=True).astype(jnp.float32)
    scale = lax.rsqrt(jnp.mean(whole * whole, axis=1, keepdims=True) + EPS)
    full_normed = (whole * scale * norm_gain[None, :]).astype(jnp.bfloat16)
    projected = jnp.dot(full_normed, weights, preferred_element_type=jnp.float32)
    rows_count = tokens.shape[0]
    projected = projected.astype(jnp.bfloat16).reshape(rows_count, 4, columns // 4)
    regrouped = lax.all_to_all(projected, ("kv", "tp"), split_axis=0, concat_axis=2, tiled=True)
    nseq = state.shape[0]
    heads = decay_rate.shape[0]
    head_dim = state.shape[2]
    props = parents.shape[1]

    def shaped(role):
        return regrouped[:, role].reshape(nseq, props, heads, head_dim)

    carried = advance(state, prev_keys, prev_values, accepted, decay_rate)
    mixed = retain(
        shaped(0),
        shaped(1),
        shaped(2),
        shaped(3),
        decay_rate,
        carried,
        parents,
        accepted,
        seq_length,
    )
    output = jnp.dot(
        lax.all_gather(mixed, ("kv", "tp"), axis=0, tiled=True),
        w_output,
        preferred_element_type=jnp.float32,
    ).astype(jnp.bfloat16)
    return (output, carried)


MESH = pl.DeviceIdType.MESH


def cos_sin(angles):
    quarter = jnp.floor(angles * (2.0 / np.pi) + 0.5)
    rest = angles - quarter * 1.5703125
    rest = rest - quarter * 4.8375129699707031e-4
    rest = rest - quarter * 7.549789948768648e-8
    sq = rest * rest
    sine = rest + rest * sq * (-1.6666654611e-1 + sq * (8.3321608736e-3 - sq * 1.9515295891e-4))
    cosine = 1.0 - 0.5 * sq + sq * sq * (
        4.166664568298827e-2 + sq * (-1.388731625493765e-3 + sq * 2.443315711809948e-5)
    )
    which = quarter.astype(jnp.int32)
    swap = (which & 1) == 1
    sin_out = jnp.where(swap, cosine, sine)
    cos_out = jnp.where(swap, sine, cosine)
    sin_out = jnp.where((which & 2) == 2, -sin_out, sin_out)
    cos_out = jnp.where(((which + 1) & 2) == 2, -cos_out, cos_out)
    return cos_out, sin_out


def swap_rows(x):
    return pltpu.roll(x, 4, axis=x.ndim - 2)


def fused(
    kv_size,
    heads,
    decay_ref,
    accepted_ref,
    parents_ref,
    length_ref,
    tokens_hbm,
    gain_hbm,
    freq_hbm,
    wq_hbm,
    wk_hbm,
    wv_hbm,
    wg_hbm,
    wo_hbm,
    state_hbm,
    pk_hbm,
    pv_hbm,
    out_hbm,
    carried_hbm,
    xg,
    gain,
    freq,
    w_all,
    w_out,
    state,
    pk,
    pv,
    carried,
    split,
    dtab,
    stab,
    stage,
    recvq,
    msend,
    mg,
    lhs,
    outb,
    local_sem,
    w_sem,
    x_send,
    x_recv,
    p_send,
    p_recv,
    m_send,
    m_recv,
):
    n = kv_size * 2
    kv, tp = lax.axis_index("kv"), lax.axis_index("tp")
    me = kv * 2 + tp
    block = xg.shape[2]
    cols = wq_hbm.shape[1]
    per = cols // 128

    def owner(dz, dt):
        return lax.rem(kv - dz + kv_size, kv_size) * 2 + (1 - tp if dt else tp)

    def target(dz, dt):
        return {"kv": lax.rem(kv + dz, kv_size), "tp": 1 - tp if dt else tp}

    near = sorted(range(1, kv_size), key=lambda d: min(d, kv_size - d))
    far = near[::-1]
    order = [(0, 0), (0, 1)] + [(d, 0) for d in near] + [(d, 1) for d in near]

    def local(src, dst, i):
        return pltpu.make_async_copy(src, dst, local_sem.at[i])

    tok_copy = local(tokens_hbm, xg.at[me], 0)
    tok_copy.start()
    small = [
        local(gain_hbm, gain, 1),
        local(freq_hbm, freq, 2),
        local(pk_hbm, pk, 3),
        local(pv_hbm, pv, 4),
        local(state_hbm, state, 5),
    ]
    for c in small:
        c.start()
    barrier = pltpu.get_barrier_semaphore()
    for dz in range(kv_size):
        for dt in range(2):
            if dz or dt:
                pl.semaphore_signal(barrier, inc=1, device_id=target(dz, dt), device_id_type=MESH)
    w_copies = []
    for t, (dz, dt) in enumerate(order):
        rows = pl.ds(pl.multiple_of(owner(dz, dt) * block, block), block)
        these = []
        for r, ref in enumerate((wq_hbm, wk_hbm, wv_hbm, wg_hbm)):
            c = pltpu.make_async_copy(
                ref.at[rows], w_all.at[rows, pl.ds(r * cols, cols)], w_sem.at[t, r]
            )
            c.start()
            these.append(c)
        w_copies.append(these)
    wo_copy = local(wo_hbm, w_out, 6)
    wo_copy.start()

    def gather_start(buf, send_sem, recv_sem):
        sends = {}
        for dz in far:
            sends[dz, 0] = pltpu.make_async_remote_copy(
                src_ref=buf.at[me], dst_ref=buf.at[me], send_sem=send_sem.at[dz],
                recv_sem=recv_sem.at[dz], device_id=target(dz, 0), device_id_type=MESH,
            )
        sends[0, 1] = pltpu.make_async_remote_copy(
            src_ref=buf.at[me], dst_ref=buf.at[me], send_sem=send_sem.at[kv_size],
            recv_sem=recv_sem.at[kv_size], device_id=target(0, 1), device_id_type=MESH,
        )
        for c in sends.values():
            c.start()
        return sends

    def relay(buf, send_sem, recv_sem, dz):
        slot = buf.at[owner(dz, 0)]
        c = pltpu.make_async_remote_copy(
            src_ref=slot, dst_ref=slot, send_sem=send_sem.at[kv_size + dz],
            recv_sem=recv_sem.at[kv_size + dz], device_id=target(0, 1), device_id_type=MESH,
        )
        c.start()
        return c

    def arrived(buf, send_sem, recv_sem, dz, dt):
        slot = buf.at[owner(dz, dt)]
        i = dz + dt * kv_size
        pltpu.make_async_remote_copy(
            src_ref=slot, dst_ref=slot, send_sem=send_sem.at[i], recv_sem=recv_sem.at[i],
            device_id=target(0, 1), device_id_type=MESH,
        ).wait_recv()

    tok_copy.wait()
    pl.semaphore_wait(barrier, n - 1)
    x_sends = gather_start(xg, x_send, x_recv)

    row = lax.broadcasted_iota(jnp.int32, (8, 128), 0)
    lane = lax.broadcasted_iota(jnp.int32, (8, 128), 1)
    which = row & 3
    low = row < 4
    props = 4
    parent = [parents_ref[0, i] for i in range(props)]
    anc = [[jnp.int32(1 if i == j else 0) for j in range(props)] for i in range(props)]
    depth = [jnp.int32(0) for i in range(props)]
    for i in range(1, props):
        for j in range(i):
            hit = jnp.where(parent[i] == j, jnp.int32(1), jnp.int32(0))
            depth[i] = depth[i] + hit * (depth[j] + 1)
            for m in range(i):
                anc[i][m] = anc[i][m] + hit * anc[j][m]

    def by_row(values):
        out = jnp.full((8, 128), values[0], jnp.int32)
        for i in range(1, props):
            out = jnp.where(which == i, jnp.full((8, 128), values[i], jnp.int32), out)
        return out.astype(jnp.float32)

    deep = by_row(depth)
    acc_count = jnp.full((8, 128), accepted_ref[0], jnp.int32).astype(jnp.float32)
    base = jnp.full((8, 128), accepted_ref[0] + length_ref[0], jnp.int32).astype(jnp.float32)
    index = which.astype(jnp.float32)
    age = jnp.maximum(acc_count - 1.0 - index, 0.0)
    live = jnp.where(index < acc_count, 1.0, 0.0)
    spacing = [jnp.maximum(deep - depth[j].astype(jnp.float32), 0.0) for j in range(props)]
    kin = [jnp.where(low, by_row([anc[i][j] for i in range(props)]), 0.0) for j in range(props)]

    for c in small:
        c.wait()
    cosine, sine = cos_sin((base + deep) * freq[...])
    row_scale = jnp.where(low, 1.0, 128.0 ** -0.5)
    cos_t = cosine * row_scale
    sin_t = jnp.where(lane < 64, -sine, sine) * row_scale

    def advance_head(h, carry):
        rate = jnp.full((8, 128), decay_ref[h], jnp.float32)
        for j in range(props):
            dtab[h, j] = kin[j] * jnp.exp(-rate * spacing[j])
        stab[h] = jnp.exp(-rate * (deep + 1.0))
        at = pl.ds(pl.multiple_of(h * 128, 128), 128)
        kh = pk[0, :, at].astype(jnp.float32)
        vh = pv[0, :, at].astype(jnp.float32)
        weighted = jnp.concatenate([kh, kh], axis=0) * (live * jnp.exp(-rate * age))
        upper = weighted.astype(jnp.bfloat16).astype(jnp.float32)
        both = jnp.where(low, upper, weighted - upper)
        v2 = jnp.concatenate([vh, vh], axis=0).astype(jnp.bfloat16)
        added = lax.dot_general(
            both.T.astype(jnp.bfloat16), v2, (((1,), (0,)), ((), ())),
            preferred_element_type=jnp.float32,
        )
        kept = jnp.exp(-rate * acc_count)[0:1]
        new = kept * state[0, h] + added
        carried[0, h] = new
        big = new.astype(jnp.bfloat16)
        split[h, :, 0:128] = big
        split[h, :, 128:256] = (new - big.astype(jnp.float32)).astype(jnp.bfloat16)
        return carry

    lax.fori_loop(0, heads, advance_head, 0, unroll=2)

    squares = jnp.zeros((xg.shape[1], 128), jnp.float32)
    total = None

    def project(total, squares, t, dz, dt):
        who = owner(dz, dt)
        for c in w_copies[t]:
            c.wait()
        x = xg[who].astype(jnp.float32)
        for q in range(block // 128):
            part = x[:, q * 128:(q + 1) * 128]
            squares = squares + part * part
        at = pl.ds(pl.multiple_of(who * block, block), block)
        xn = (x * gain[:, at]).astype(jnp.bfloat16)
        y = jnp.dot(xn, w_all[at, :], preferred_element_type=jnp.float32)
        return (y if total is None else total + y), squares

    total, squares = project(total, squares, 0, 0, 0)
    arrived(xg, x_send, x_recv, 0, 1)
    total, squares = project(total, squares, 1, 0, 1)
    relays = []
    waited = set()
    for t, (dz, dt) in enumerate(order):
        if t < 2:
            continue
        if dt == 0:
            for d in (near[:2] if dz in near[:2] else [dz]):
                if d not in waited:
                    waited.add(d)
                    arrived(xg, x_send, x_recv, d, 0)
                    relays.append(relay(xg, x_send, x_recv, d))
        else:
            arrived(xg, x_send, x_recv, dz, 1)
        total, squares = project(total, squares, t, dz, dt)
    width = block * n
    scale = lax.rsqrt(jnp.sum(squares, axis=1, keepdims=True) * (1.0 / width) + EPS)
    total = total * scale
    low_c = lax.broadcasted_iota(jnp.int32, (8, cols), 0) < 4
    for t in range(n // 2):
        q, k, v, g = [total[8 * t:8 * t + 8, r * cols:(r + 1) * cols] for r in range(4)]
        stage[2 * t] = jnp.concatenate(
            [jnp.where(low_c, q, swap_rows(k)), jnp.where(low_c, v, swap_rows(g))], axis=0
        ).astype(jnp.bfloat16)
        stage[2 * t + 1] = jnp.concatenate(
            [jnp.where(low_c, swap_rows(q), k), jnp.where(low_c, swap_rows(v), g)], axis=0
        ).astype(jnp.bfloat16)
    p_sends = []
    for dz in far + [0]:
        for dt in range(2):
            if dz or dt:
                to = target(dz, dt)
                c = pltpu.make_async_remote_copy(
                    src_ref=stage.at[to["kv"] * 2 + to["tp"]], dst_ref=recvq.at[me],
                    send_sem=p_send.at[dz * 2 + dt], recv_sem=p_recv.at[dz * 2 + dt],
                    device_id=to, device_id_type=MESH,
                )
                c.start()
                p_sends.append(c)
    recvq[me] = stage[me]
    carried_copy = local(carried, carried_hbm, 7)
    carried_copy.start()
    wo_copy.wait()
    for dz in range(kv_size):
        for dt in range(2):
            if dz or dt:
                slot = recvq.at[owner(dz, dt)]
                i = dz * 2 + dt
                pltpu.make_async_remote_copy(
                    src_ref=slot, dst_ref=slot, send_sem=p_send.at[i], recv_sem=p_recv.at[i],
                    device_id=target(0, 1), device_id_type=MESH,
                ).wait_recv()

    low3 = low[None]
    for k in range(per):
        got = recvq[:, :, k * 128:(k + 1) * 128].astype(jnp.float32)
        qk, vg = got[:, 0:8], got[:, 8:16]
        turned = qk * cos_t[None] + pltpu.roll(qk, 64, axis=2) * sin_t[None]
        mine = [dtab[s * per + k] for s in range(n)]
        decay = jnp.stack([stab[s * per + k] for s in range(n)])
        qs = turned * decay
        qs = jnp.where(low3, qs, swap_rows(qs))
        upper = qs.astype(jnp.bfloat16).astype(jnp.float32)
        pair = jnp.where(low3, upper, qs - upper).astype(jnp.bfloat16)
        raws = []
        for s in range(n):
            y = jnp.dot(pair[s], split[s * per + k], preferred_element_type=jnp.float32)
            raws.append(y[:, 0:128] + y[:, 128:256])
        raw = jnp.stack(raws)
        raw = raw + swap_rows(raw)
        for j in range(props):
            score = jnp.sum(turned * turned[:, 4 + j:5 + j, :], axis=2, keepdims=True)
            raw = raw + score * jnp.stack([m[j] for m in mine]) * vg[:, j:j + 1, :]
        centred = raw - jnp.sum(raw, axis=2, keepdims=True) * (1.0 / 128)
        spread = jnp.sum(centred * centred, axis=2, keepdims=True) * (1.0 / 128)
        gate = swap_rows(vg)
        mixed = centred * lax.rsqrt(spread + EPS) * (gate / (1.0 + jnp.exp(-gate)))
        group = n // 4
        for b in range(group):
            first = jnp.where(low, mixed[b], swap_rows(mixed[group + b]))
            second = jnp.where(low, mixed[2 * group + b], swap_rows(mixed[3 * group + b]))
            at = b * cols + k * 128
            mg[me, :, at:at + 128] = jnp.concatenate([first, second], axis=0).astype(jnp.bfloat16)

    m_sends = gather_start(mg, m_send, m_recv)
    m_relays = []
    for dz in near:
        arrived(mg, m_send, m_recv, dz, 0)
        m_relays.append(relay(mg, m_send, m_recv, dz))
    arrived(mg, m_send, m_recv, 0, 1)
    for dz in near:
        arrived(mg, m_send, m_recv, dz, 1)
    chunk = mg.shape[2]
    low_m = lax.broadcasted_iota(jnp.int32, (8, chunk), 0) < 4
    for t in range(n // 2):
        one = mg[2 * t].astype(jnp.float32)
        two = mg[2 * t + 1].astype(jnp.float32)
        for c in range(4):
            at = 8 * (c // 2)
            a, b = one[at:at + 8], two[at:at + 8]
            if c % 2 == 0:
                piece = jnp.where(low_m, a, swap_rows(b))
            else:
                piece = jnp.where(low_m, swap_rows(a), b)
            lhs[8 * t:8 * t + 8, c * chunk:(c + 1) * chunk] = piece
    outb[...] = jnp.dot(
        lhs[...].astype(jnp.bfloat16), w_out[...], preferred_element_type=jnp.float32
    ).astype(jnp.bfloat16)
    out_copy = local(outb, out_hbm, 8)
    out_copy.start()
    for c in list(x_sends.values()) + relays + p_sends + list(m_sends.values()) + m_relays:
        c.wait_send()
    carried_copy.wait()
    out_copy.wait()


def fused_device(
    kv_size, tokens, norm_gain, w_query, w_key, w_value, w_gate, w_output, decay_rate, state,
    prev_keys, prev_values, accepted, parents, seq_length,
):
    n = kv_size * 2
    rows, block = tokens.shape
    width, cols = w_query.shape
    heads = decay_rate.shape[0]
    hid, out_cols = w_output.shape
    freq = 10000.0 ** (-(np.arange(128) % 64) / 64.0)
    freq = jnp.asarray(freq.astype(np.float32)[None, :])
    smem = pl.BlockSpec(memory_space=pltpu.SMEM)
    hbm = pl.BlockSpec(memory_space=pl.ANY)
    bf, f32 = jnp.bfloat16, jnp.float32
    dma = pltpu.SemaphoreType.DMA
    return pl.pallas_call(
        functools.partial(fused, kv_size, heads),
        out_shape=(
            jax.ShapeDtypeStruct((rows, out_cols), bf),
            jax.ShapeDtypeStruct(state.shape, f32),
        ),
        in_specs=[smem] * 4 + [hbm] * 11,
        out_specs=(hbm, hbm),
        scratch_shapes=[
            pltpu.VMEM((n, rows, block), bf),
            pltpu.VMEM((1, width), f32),
            pltpu.VMEM((1, 128), f32),
            pltpu.VMEM((width, 4 * cols), bf),
            pltpu.VMEM((hid, out_cols), bf),
            pltpu.VMEM(state.shape, f32),
            pltpu.VMEM(prev_keys.shape, bf),
            pltpu.VMEM(prev_values.shape, bf),
            pltpu.VMEM(state.shape, f32),
            pltpu.VMEM((heads, 128, 256), bf),
            pltpu.VMEM((heads, 4, 8, 128), f32),
            pltpu.VMEM((heads, 8, 128), f32),
            pltpu.VMEM((n, 16, cols), bf),
            pltpu.VMEM((n, 16, cols), bf),
            pltpu.VMEM((16, hid // 4), bf),
            pltpu.VMEM((n, 16, hid // 4), bf),
            pltpu.VMEM((rows, hid), f32),
            pltpu.VMEM((rows, out_cols), bf),
            dma((9,)),
            dma((n, 4)),
            dma((n,)),
            dma((n,)),
            dma((n,)),
            dma((n,)),
            dma((n,)),
            dma((n,)),
        ],
        compiler_params=pltpu.CompilerParams(
            collective_id=0, has_side_effects=True, vmem_limit_bytes=60 * 1024 * 1024
        ),
    )(
        decay_rate, accepted, parents, seq_length, tokens, norm_gain[None, :], freq, w_query,
        w_key, w_value, w_gate, w_output, state, prev_keys, prev_values,
    )


def choose(kv_size, tp_size, *args):
    tokens, w_query, state, parents = args[0], args[2], args[8], args[12]
    n = kv_size * tp_size
    fits = (
        tp_size == 2
        and n % 4 == 0
        and kv_size > 2
        and state.shape[0] == 1
        and state.shape[2:] == (128, 128)
        and parents.shape[1] == 4
        and w_query.shape[1] % 128 == 0
        and tokens.shape[0] == 4 * n
        and tokens.shape[1] % 128 == 0
    )
    if fits:
        return fused_device(kv_size, *args)
    return per_device(*args)


def solution(mesh):
    placed = (
        P("dp", ("kv", "tp")),
        P(),
        P(None, ("kv", "tp")),
        P(None, ("kv", "tp")),
        P(None, ("kv", "tp")),
        P(None, ("kv", "tp")),
        P(None, ("kv", "tp")),
        P(),
        P(("dp", "kv", "tp"), None, None, None),
        P(("dp", "kv", "tp"), None, None),
        P(("dp", "kv", "tp"), None, None),
        P(("dp", "kv", "tp")),
        P(("dp", "kv", "tp"), None),
        P(("dp", "kv", "tp")),
    )
    return jax.shard_map(
        functools.partial(choose, mesh.shape["kv"], mesh.shape["tp"]),
        mesh=mesh,
        in_specs=placed,
        out_specs=(P("dp", ("kv", "tp")), P(("dp", "kv", "tp"), None, None, None)),
        check_vma=False,
    )
```

```python
import functools

import jax
import jax.numpy as jnp
import numpy as np
from jax import lax
from jax.experimental import pallas as pl
from jax.experimental.pallas import tpu as pltpu
from jax.sharding import PartitionSpec as P

EPS = 1e-06
HIGH = lax.Precision.HIGHEST


def rotate(tensor, positions):
    half_dim = tensor.shape[-1] // 2
    frequency = 10000.0 ** (-jnp.arange(half_dim, dtype=jnp.float32) / half_dim)
    angles = positions[:, :, None] * frequency[None, None, :]
    cosine = jnp.cos(angles)[:, :, None, :]
    sine_part = jnp.sin(angles)[:, :, None, :]
    first = tensor[..., :half_dim]
    second = tensor[..., half_dim:]
    return jnp.concatenate(
        [first * cosine - second * sine_part, second * cosine + first * sine_part], axis=-1
    )


def ancestry_of(parents):
    props = parents.shape[1]
    linked = (parents[:, :, None] == jnp.arange(props, dtype=jnp.int32)[None, None, :]).astype(
        jnp.float32
    )
    identity = jnp.broadcast_to(jnp.eye(props, dtype=jnp.float32), linked.shape)
    ancestry = identity
    power = identity
    for hop in range(props - 1):
        power = jnp.einsum("bij,bjk->bik", power, linked, precision=HIGH)
        ancestry = ancestry + power
    depths = jnp.sum(ancestry, axis=-1) - 1.0
    return (ancestry, depths)


def advance(state, prev_keys, prev_values, accepted, decays):
    nseq, props, width = prev_keys.shape
    heads = decays.shape[0]
    head_dim = width // heads
    old_keys = prev_keys.astype(jnp.float32).reshape(nseq, props, heads, head_dim)
    old_values = prev_values.astype(jnp.float32).reshape(nseq, props, heads, head_dim)
    steps_done = accepted.astype(jnp.float32)[:, None]
    index = jnp.arange(props, dtype=jnp.float32)[None, :]
    age = jnp.maximum(steps_done - 1.0 - index, 0.0)
    weights = jnp.where(
        (index < steps_done)[:, :, None], jnp.exp(-decays[None, None, :] * age[:, :, None]), 0.0
    )
    kept = jnp.exp(-decays[None, :] * steps_done)
    added = jnp.einsum("bphd,bphe->bhde", old_keys * weights[..., None], old_values, precision=HIGH)
    return kept[:, :, None, None] * state + added


def retain(queries, key_rows, val_rows, gate_rows, decays, carried, parents, accepted, seq_length):
    nseq, props, heads, head_dim = queries.shape
    ancestry, depths = ancestry_of(parents)
    positions = (seq_length + accepted).astype(jnp.float32)[:, None] + depths
    rotated_q = rotate(queries.astype(jnp.float32), positions)
    rotated_k = rotate(key_rows.astype(jnp.float32), positions) * head_dim ** (-0.5)
    scores = jnp.einsum("bihd,bjhd->bhij", rotated_q, rotated_k, precision=HIGH)
    spacing = jnp.maximum(depths[:, :, None] - depths[:, None, :], 0.0)
    weighting = ancestry[:, None] * jnp.exp(-decays[None, :, None, None] * spacing[:, None])
    within = jnp.einsum(
        "bhij,bjhe->bihe", scores * weighting, val_rows.astype(jnp.float32), precision=HIGH
    )
    state_scale = jnp.exp(-decays[None, None, :] * (depths[:, :, None] + 1.0))
    from_state = (
        jnp.einsum("bihd,bhde->bihe", rotated_q, carried, precision=HIGH) * state_scale[..., None]
    )
    mixed_raw = within + from_state
    average = jnp.mean(mixed_raw, axis=-1, keepdims=True)
    centred = mixed_raw - average
    variance = jnp.mean(centred * centred, axis=-1, keepdims=True)
    normed = (centred * lax.rsqrt(variance + EPS)).reshape(nseq * props, heads * head_dim)
    gates = gate_rows.astype(jnp.float32).reshape(nseq * props, heads * head_dim)
    return (normed * jax.nn.silu(gates)).astype(jnp.bfloat16)


def per_device(
    tokens,
    norm_gain,
    w_query,
    w_key,
    w_value,
    w_gate,
    w_output,
    decay_rate,
    state,
    prev_keys,
    prev_values,
    accepted,
    parents,
    seq_length,
):
    weights = jnp.concatenate([w_query, w_key, w_value, w_gate], axis=1)
    columns = weights.shape[1]
    whole = lax.all_gather(tokens, ("kv", "tp"), axis=1, tiled=True).astype(jnp.float32)
    scale = lax.rsqrt(jnp.mean(whole * whole, axis=1, keepdims=True) + EPS)
    full_normed = (whole * scale * norm_gain[None, :]).astype(jnp.bfloat16)
    projected = jnp.dot(full_normed, weights, preferred_element_type=jnp.float32)
    rows_count = tokens.shape[0]
    projected = projected.astype(jnp.bfloat16).reshape(rows_count, 4, columns // 4)
    regrouped = lax.all_to_all(projected, ("kv", "tp"), split_axis=0, concat_axis=2, tiled=True)
    nseq = state.shape[0]
    heads = decay_rate.shape[0]
    head_dim = state.shape[2]
    props = parents.shape[1]

    def shaped(role):
        return regrouped[:, role].reshape(nseq, props, heads, head_dim)

    carried = advance(state, prev_keys, prev_values, accepted, decay_rate)
    mixed = retain(
        shaped(0),
        shaped(1),
        shaped(2),
        shaped(3),
        decay_rate,
        carried,
        parents,
        accepted,
        seq_length,
    )
    output = jnp.dot(
        lax.all_gather(mixed, ("kv", "tp"), axis=0, tiled=True),
        w_output,
        preferred_element_type=jnp.float32,
    ).astype(jnp.bfloat16)
    return (output, carried)


MESH = pl.DeviceIdType.MESH


def cos_sin(angles):
    quarter = jnp.floor(angles * (2.0 / np.pi) + 0.5)
    rest = angles - quarter * 1.5703125
    rest = rest - quarter * 4.8375129699707031e-4
    rest = rest - quarter * 7.549789948768648e-8
    sq = rest * rest
    sine = rest + rest * sq * (-1.6666654611e-1 + sq * (8.3321608736e-3 - sq * 1.9515295891e-4))
    cosine = 1.0 - 0.5 * sq + sq * sq * (
        4.166664568298827e-2 + sq * (-1.388731625493765e-3 + sq * 2.443315711809948e-5)
    )
    which = quarter.astype(jnp.int32)
    swap = (which & 1) == 1
    sin_out = jnp.where(swap, cosine, sine)
    cos_out = jnp.where(swap, sine, cosine)
    sin_out = jnp.where((which & 2) == 2, -sin_out, sin_out)
    cos_out = jnp.where(((which + 1) & 2) == 2, -cos_out, cos_out)
    return cos_out, sin_out


def swap_rows(x):
    return pltpu.roll(x, 4, axis=x.ndim - 2)


def fused(
    kv_size,
    heads,
    decay_hbm,
    accepted_hbm,
    parents_hbm,
    length_hbm,
    tokens_hbm,
    gain_hbm,
    freq_hbm,
    wq_hbm,
    wk_hbm,
    wv_hbm,
    wg_hbm,
    wo_hbm,
    state_hbm,
    pk_hbm,
    pv_hbm,
    mg,
    carried,
    w_out,
    xg,
    gain,
    freq,
    w_all,
    state,
    pk,
    pv,
    split,
    dtab,
    stab,
    stage,
    recvq,
    decay_ref,
    accepted_ref,
    parents_ref,
    length_ref,
    local_sem,
    w_sem,
    x_send,
    x_recv,
    p_send,
    p_recv,
    m_send,
    m_recv,
):
    n = kv_size * 2
    kv, tp = lax.axis_index("kv"), lax.axis_index("tp")
    me = kv * 2 + tp
    block = xg.shape[2]
    cols = wq_hbm.shape[1]
    per = cols // 128

    ranked = [sorted(range(kv_size), key=lambda o: abs(o - z)) for z in range(kv_size)]
    seat = [
        sum(jnp.where(kv == z, ranked[z][d], 0) for z in range(kv_size)) for d in range(kv_size)
    ]

    def owner(d, dt):
        return seat[d] * 2 + (1 - tp if dt else tp)

    def target(d, dt):
        return {"kv": seat[d], "tp": 1 - tp if dt else tp}

    near = list(range(1, kv_size))
    far = near[::-1]
    order = [(0, 0), (0, 1)] + [(d, 0) for d in near] + [(d, 1) for d in near]

    def local(src, dst, i):
        return pltpu.make_async_copy(src, dst, local_sem.at[i])

    barrier = pltpu.get_barrier_semaphore()
    for dz in range(kv_size):
        for dt in range(2):
            if dz or dt:
                pl.semaphore_signal(barrier, inc=1, device_id=target(dz, dt), device_id_type=MESH)
    tok_copy = local(tokens_hbm, xg.at[me], 0)
    tok_copy.start()
    scalars = [
        local(decay_hbm, decay_ref, 7),
        local(accepted_hbm, accepted_ref, 8),
        local(parents_hbm, parents_ref, 9),
        local(length_hbm, length_ref, 10),
    ]
    for c in scalars:
        c.start()
    small = [
        local(gain_hbm, gain, 1),
        local(freq_hbm, freq, 2),
        local(pk_hbm, pk, 3),
        local(pv_hbm, pv, 4),
    ]
    for c in small:
        c.start()
    small.append(local(state_hbm, state, 5))
    w_copies = []
    for t, (dz, dt) in enumerate(order):
        rows = pl.ds(pl.multiple_of(owner(dz, dt) * block, block), block)
        these = []
        for r, ref in enumerate((wq_hbm, wk_hbm, wv_hbm, wg_hbm)):
            c = pltpu.make_async_copy(
                ref.at[rows], w_all.at[rows, pl.ds(r * cols, cols)], w_sem.at[t, r]
            )
            these.append(c)
        w_copies.append(these)
    wo_copy = local(wo_hbm, w_out, 6)

    def load(t):
        for c in w_copies[t]:
            c.start()


    def gather_start(buf, send_sem, recv_sem):
        sends = {}
        for dz in far:
            sends[dz, 0] = pltpu.make_async_remote_copy(
                src_ref=buf.at[me], dst_ref=buf.at[me], send_sem=send_sem.at[dz],
                recv_sem=recv_sem.at[kv], device_id=target(dz, 0), device_id_type=MESH,
            )
        sends[0, 1] = pltpu.make_async_remote_copy(
            src_ref=buf.at[me], dst_ref=buf.at[me], send_sem=send_sem.at[kv_size],
            recv_sem=recv_sem.at[kv_size + kv], device_id=target(0, 1), device_id_type=MESH,
        )
        for c in sends.values():
            c.start()
        return sends

    def relay(buf, send_sem, recv_sem, dz):
        slot = buf.at[owner(dz, 0)]
        c = pltpu.make_async_remote_copy(
            src_ref=slot, dst_ref=slot, send_sem=send_sem.at[kv_size + dz],
            recv_sem=recv_sem.at[kv_size + seat[dz]], device_id=target(0, 1), device_id_type=MESH,
        )
        c.start()
        return c

    def arrived(buf, send_sem, recv_sem, dz, dt):
        slot = buf.at[owner(dz, dt)]
        i = seat[dz] + dt * kv_size
        pltpu.make_async_remote_copy(
            src_ref=slot, dst_ref=slot, send_sem=send_sem.at[i], recv_sem=recv_sem.at[i],
            device_id=target(0, 1), device_id_type=MESH,
        ).wait_recv()

    tok_copy.wait()
    for t in range(2):
        load(t)
    pl.semaphore_wait(barrier, n - 1)
    x_sends = gather_start(xg, x_send, x_recv)
    for t in range(2, n):
        load(t)
    small[-1].start()

    for c in scalars:
        c.wait()
    row = lax.broadcasted_iota(jnp.int32, (8, 128), 0)
    lane = lax.broadcasted_iota(jnp.int32, (8, 128), 1)
    which = row & 3
    low = row < 4
    props = 4
    parent = [parents_ref[0, i] for i in range(props)]
    anc = [[jnp.int32(1 if i == j else 0) for j in range(props)] for i in range(props)]
    depth = [jnp.int32(0) for i in range(props)]
    for i in range(1, props):
        for j in range(i):
            hit = jnp.where(parent[i] == j, jnp.int32(1), jnp.int32(0))
            depth[i] = depth[i] + hit * (depth[j] + 1)
            for m in range(i):
                anc[i][m] = anc[i][m] + hit * anc[j][m]

    def by_row(values):
        out = jnp.full((8, 128), values[0], jnp.int32)
        for i in range(1, props):
            out = jnp.where(which == i, jnp.full((8, 128), values[i], jnp.int32), out)
        return out.astype(jnp.float32)

    deep = by_row(depth)
    acc_count = jnp.full((8, 128), accepted_ref[0, 0], jnp.int32).astype(jnp.float32)
    base = jnp.full((8, 128), accepted_ref[0, 0] + length_ref[0, 0], jnp.int32).astype(jnp.float32)
    index = which.astype(jnp.float32)
    age = jnp.maximum(acc_count - 1.0 - index, 0.0)
    live = jnp.where(index < acc_count, 1.0, 0.0)
    spacing = [jnp.maximum(deep - depth[j].astype(jnp.float32), 0.0) for j in range(props)]
    kin = [jnp.where(low, by_row([anc[i][j] for i in range(props)]), 0.0) for j in range(props)]

    for c in small[:-1]:
        c.wait()
    cosine, sine = cos_sin((base + deep) * freq[...])
    row_scale = jnp.where(low, 1.0, 128.0 ** -0.5)
    cos_t = cosine * row_scale
    sin_t = jnp.where(lane < 64, -sine, sine) * row_scale

    squares = jnp.zeros((xg.shape[1], 128), jnp.float32)
    total = None

    def project(total, squares, t, dz, dt):
        who = owner(dz, dt)
        for c in w_copies[t]:
            c.wait()
        x = xg[who].astype(jnp.float32)
        for q in range(block // 128):
            part = x[:, q * 128:(q + 1) * 128]
            squares = squares + part * part
        at = pl.ds(pl.multiple_of(who * block, block), block)
        xn = (x * gain[:, at]).astype(jnp.bfloat16)
        y = jnp.dot(xn, w_all[at, :], preferred_element_type=jnp.float32)
        return (y if total is None else total + y), squares

    total, squares = project(total, squares, 0, 0, 0)
    arrived(xg, x_send, x_recv, 0, 1)
    total, squares = project(total, squares, 1, 0, 1)
    relays = []
    waited = set()
    for t, (dz, dt) in enumerate(order):
        if t < 2:
            continue
        if dt == 0:
            for d in (near[:2] if dz in near[:2] else [dz]):
                if d not in waited:
                    waited.add(d)
                    arrived(xg, x_send, x_recv, d, 0)
                    relays.append(relay(xg, x_send, x_recv, d))
        else:
            arrived(xg, x_send, x_recv, dz, 1)
        total, squares = project(total, squares, t, dz, dt)
    width = block * n
    scale = lax.rsqrt(jnp.sum(squares, axis=1, keepdims=True) * (1.0 / width) + EPS)
    total = total * scale
    low_c = lax.broadcasted_iota(jnp.int32, (8, cols), 0) < 4
    for t in range(n // 2):
        q, k, v, g = [total[8 * t:8 * t + 8, r * cols:(r + 1) * cols] for r in range(4)]
        stage[2 * t] = jnp.concatenate(
            [jnp.where(low_c, q, swap_rows(k)), jnp.where(low_c, v, swap_rows(g))], axis=0
        ).astype(jnp.bfloat16)
        stage[2 * t + 1] = jnp.concatenate(
            [jnp.where(low_c, swap_rows(q), k), jnp.where(low_c, swap_rows(v), g)], axis=0
        ).astype(jnp.bfloat16)
    p_sends = []
    for dz in far + [0]:
        for dt in range(2):
            if dz or dt:
                to = target(dz, dt)
                c = pltpu.make_async_remote_copy(
                    src_ref=stage.at[to["kv"] * 2 + to["tp"]], dst_ref=recvq.at[me],
                    send_sem=p_send.at[dz * 2 + dt], recv_sem=p_recv.at[me],
                    device_id=to, device_id_type=MESH,
                )
                c.start()
                p_sends.append(c)
    wo_copy.start()
    recvq[me] = stage[me]
    small[-1].wait()

    def advance_head(h, carry):
        rate = jnp.full((8, 128), decay_ref[h], jnp.float32)
        for j in range(props):
            dtab[h, j] = kin[j] * jnp.exp(-rate * spacing[j])
        stab[h] = jnp.exp(-rate * (deep + 1.0))
        at = pl.ds(pl.multiple_of(h * 128, 128), 128)
        kh = pk[0, :, at].astype(jnp.float32)
        vh = pv[0, :, at].astype(jnp.float32)
        weighted = jnp.concatenate([kh, kh], axis=0) * (live * jnp.exp(-rate * age))
        upper = weighted.astype(jnp.bfloat16).astype(jnp.float32)
        both = jnp.where(low, upper, weighted - upper)
        v2 = jnp.concatenate([vh, vh], axis=0).astype(jnp.bfloat16)
        added = lax.dot_general(
            both.T.astype(jnp.bfloat16), v2, (((1,), (0,)), ((), ())),
            preferred_element_type=jnp.float32,
        )
        kept = jnp.exp(-rate * acc_count)[0:1]
        new = kept * state[0, h] + added
        carried[0, h] = new
        big = new.astype(jnp.bfloat16)
        split[h, :, 0:128] = big
        split[h, :, 128:256] = (new - big.astype(jnp.float32)).astype(jnp.bfloat16)
        return carry

    lax.fori_loop(0, heads, advance_head, 0, unroll=2)

    for dz in range(kv_size):
        for dt in range(2):
            if dz or dt:
                slot = recvq.at[owner(dz, dt)]
                i = owner(dz, dt)
                pltpu.make_async_remote_copy(
                    src_ref=slot, dst_ref=slot, send_sem=p_send.at[i], recv_sem=p_recv.at[i],
                    device_id=target(0, 1), device_id_type=MESH,
                ).wait_recv()

    low3 = low[None]
    for k in range(per):
        got = recvq[:, :, k * 128:(k + 1) * 128].astype(jnp.float32)
        qk, vg = got[:, 0:8], got[:, 8:16]
        turned = qk * cos_t[None] + pltpu.roll(qk, 64, axis=2) * sin_t[None]
        mine = [dtab[s * per + k] for s in range(n)]
        decay = jnp.stack([stab[s * per + k] for s in range(n)])
        qs = turned * decay
        qs = jnp.where(low3, qs, swap_rows(qs))
        upper = qs.astype(jnp.bfloat16).astype(jnp.float32)
        pair = jnp.where(low3, upper, qs - upper).astype(jnp.bfloat16)
        raws = []
        for s in range(n):
            y = jnp.dot(pair[s], split[s * per + k], preferred_element_type=jnp.float32)
            raws.append(y[:, 0:128] + y[:, 128:256])
        raw = jnp.stack(raws)
        raw = raw + swap_rows(raw)
        for j in range(props):
            score = jnp.sum(turned * turned[:, 4 + j:5 + j, :], axis=2, keepdims=True)
            raw = raw + score * jnp.stack([m[j] for m in mine]) * vg[:, j:j + 1, :]
        centred = raw - jnp.sum(raw, axis=2, keepdims=True) * (1.0 / 128)
        spread = jnp.sum(centred * centred, axis=2, keepdims=True) * (1.0 / 128)
        gate = swap_rows(vg)
        mixed = centred * lax.rsqrt(spread + EPS) * (gate / (1.0 + jnp.exp(-gate)))
        group = n // 4
        for b in range(group):
            first = jnp.where(low, mixed[b], swap_rows(mixed[group + b]))
            second = jnp.where(low, mixed[2 * group + b], swap_rows(mixed[3 * group + b]))
            at = b * cols + k * 128
            mg[me, :, at:at + 128] = jnp.concatenate([first, second], axis=0).astype(jnp.bfloat16)

    m_sends = gather_start(mg, m_send, m_recv)
    m_relays = []
    for dz in near:
        arrived(mg, m_send, m_recv, dz, 0)
        m_relays.append(relay(mg, m_send, m_recv, dz))
    arrived(mg, m_send, m_recv, 0, 1)
    for dz in near:
        arrived(mg, m_send, m_recv, dz, 1)
    wo_copy.wait()
    for c in list(x_sends.values()) + relays + p_sends + list(m_sends.values()) + m_relays:
        c.wait_send()


def finish(mg, carried, w_out, out_hbm, carried_hbm, lhs, outb, sem):
    carried_copy = pltpu.make_async_copy(carried, carried_hbm, sem.at[0])
    carried_copy.start()
    chunk = mg.shape[2]
    low_m = lax.broadcasted_iota(jnp.int32, (8, chunk), 0) < 4
    for t in range(mg.shape[0] // 2):
        one = mg[2 * t].astype(jnp.float32)
        two = mg[2 * t + 1].astype(jnp.float32)
        for c in range(4):
            at = 8 * (c // 2)
            a, b = one[at:at + 8], two[at:at + 8]
            if c % 2 == 0:
                piece = jnp.where(low_m, a, swap_rows(b))
            else:
                piece = jnp.where(low_m, swap_rows(a), b)
            lhs[8 * t:8 * t + 8, c * chunk:(c + 1) * chunk] = piece
    outb[...] = jnp.dot(
        lhs[...].astype(jnp.bfloat16), w_out[...], preferred_element_type=jnp.float32
    ).astype(jnp.bfloat16)
    out_copy = pltpu.make_async_copy(outb, out_hbm, sem.at[1])
    out_copy.start()
    out_copy.wait()
    carried_copy.wait()


def fused_device(
    kv_size, tokens, norm_gain, w_query, w_key, w_value, w_gate, w_output, decay_rate, state,
    prev_keys, prev_values, accepted, parents, seq_length,
):
    n = kv_size * 2
    rows, block = tokens.shape
    width, cols = w_query.shape
    heads = decay_rate.shape[0]
    hid, out_cols = w_output.shape
    freq = 10000.0 ** (-(np.arange(128) % 64) / 64.0)
    freq = jnp.asarray(freq.astype(np.float32)[None, :])
    hbm = pl.BlockSpec(memory_space=pltpu.HBM)
    vmem = pl.BlockSpec(memory_space=pltpu.VMEM)
    bf, f32 = jnp.bfloat16, jnp.float32
    dma = pltpu.SemaphoreType.DMA
    room = 67043328 - state.size * 4 - hid * out_cols * 2 - n * 16 * (hid // 4) * 2
    gathered, new_state, w_near = pl.pallas_call(
        functools.partial(fused, kv_size, heads),
        out_shape=(
            pltpu.VMEM((n, 16, hid // 4), bf),
            pltpu.VMEM(state.shape, f32),
            pltpu.VMEM((hid, out_cols), bf),
        ),
        in_specs=[hbm] * 15,
        out_specs=(vmem, vmem, vmem),
        scratch_shapes=[
            pltpu.VMEM((n, rows, block), bf),
            pltpu.VMEM((1, width), f32),
            pltpu.VMEM((1, 128), f32),
            pltpu.VMEM((width, 4 * cols), bf),
            pltpu.VMEM(state.shape, f32),
            pltpu.VMEM(prev_keys.shape, bf),
            pltpu.VMEM(prev_values.shape, bf),
            pltpu.VMEM((heads, 128, 256), bf),
            pltpu.VMEM((heads, 4, 8, 128), f32),
            pltpu.VMEM((heads, 8, 128), f32),
            pltpu.VMEM((n, 16, cols), bf),
            pltpu.VMEM((n, 16, cols), bf),
            pltpu.SMEM(decay_rate.shape, f32),
            pltpu.SMEM((1, 1), jnp.int32),
            pltpu.SMEM(parents.shape, jnp.int32),
            pltpu.SMEM((1, 1), jnp.int32),
            dma((11,)),
            dma((n, 4)),
            dma((n,)),
            dma((n,)),
            dma((n,)),
            dma((n,)),
            dma((n,)),
            dma((n,)),
        ],
        compiler_params=pltpu.CompilerParams(
            collective_id=0, has_side_effects=True, vmem_limit_bytes=room
        ),
    )(
        decay_rate, accepted[None, :], parents, seq_length[None, :], tokens, norm_gain[None, :], freq, w_query,
        w_key, w_value, w_gate, w_output, state, prev_keys, prev_values,
    )
    return pl.pallas_call(
        finish,
        out_shape=(
            jax.ShapeDtypeStruct((rows, out_cols), bf),
            jax.ShapeDtypeStruct(state.shape, f32),
        ),
        in_specs=[vmem] * 3,
        out_specs=(hbm, hbm),
        scratch_shapes=[
            pltpu.VMEM((rows, hid), f32),
            pltpu.VMEM((rows, out_cols), bf),
            dma((2,)),
        ],
        compiler_params=pltpu.CompilerParams(vmem_limit_bytes=8 * 1024 * 1024),
    )(gathered, new_state, w_near)


def choose(kv_size, tp_size, *args):
    tokens, w_query, state, parents = args[0], args[2], args[8], args[12]
    n = kv_size * tp_size
    fits = (
        tp_size == 2
        and n % 4 == 0
        and kv_size > 2
        and state.shape[0] == 1
        and state.shape[2:] == (128, 128)
        and parents.shape[1] == 4
        and w_query.shape[1] % 128 == 0
        and tokens.shape[0] == 4 * n
        and tokens.shape[1] % 128 == 0
    )
    if fits:
        return fused_device(kv_size, *args)
    return per_device(*args)


def solution(mesh):
    placed = (
        P("dp", ("kv", "tp")),
        P(),
        P(None, ("kv", "tp")),
        P(None, ("kv", "tp")),
        P(None, ("kv", "tp")),
        P(None, ("kv", "tp")),
        P(None, ("kv", "tp")),
        P(),
        P(("dp", "kv", "tp"), None, None, None),
        P(("dp", "kv", "tp"), None, None),
        P(("dp", "kv", "tp"), None, None),
        P(("dp", "kv", "tp")),
        P(("dp", "kv", "tp"), None),
        P(("dp", "kv", "tp")),
    )
    return jax.shard_map(
        functools.partial(choose, mesh.shape["kv"], mesh.shape["tp"]),
        mesh=mesh,
        in_specs=placed,
        out_specs=(P("dp", ("kv", "tp")), P(("dp", "kv", "tp"), None, None, None)),
        check_vma=False,
    )
```

```python
import functools

import jax
import jax.numpy as jnp
import numpy as np
from jax import lax
from jax.experimental import pallas as pl
from jax.experimental.pallas import tpu as pltpu
from jax.sharding import PartitionSpec as P

EPS = 1e-06
HIGH = lax.Precision.HIGHEST


def rotate(tensor, positions):
    half_dim = tensor.shape[-1] // 2
    frequency = 10000.0 ** (-jnp.arange(half_dim, dtype=jnp.float32) / half_dim)
    angles = positions[:, :, None] * frequency[None, None, :]
    cosine = jnp.cos(angles)[:, :, None, :]
    sine_part = jnp.sin(angles)[:, :, None, :]
    first = tensor[..., :half_dim]
    second = tensor[..., half_dim:]
    return jnp.concatenate(
        [first * cosine - second * sine_part, second * cosine + first * sine_part], axis=-1
    )


def ancestry_of(parents):
    props = parents.shape[1]
    linked = (parents[:, :, None] == jnp.arange(props, dtype=jnp.int32)[None, None, :]).astype(
        jnp.float32
    )
    identity = jnp.broadcast_to(jnp.eye(props, dtype=jnp.float32), linked.shape)
    ancestry = identity
    power = identity
    for hop in range(props - 1):
        power = jnp.einsum("bij,bjk->bik", power, linked, precision=HIGH)
        ancestry = ancestry + power
    depths = jnp.sum(ancestry, axis=-1) - 1.0
    return (ancestry, depths)


def advance(state, prev_keys, prev_values, accepted, decays):
    nseq, props, width = prev_keys.shape
    heads = decays.shape[0]
    head_dim = width // heads
    old_keys = prev_keys.astype(jnp.float32).reshape(nseq, props, heads, head_dim)
    old_values = prev_values.astype(jnp.float32).reshape(nseq, props, heads, head_dim)
    steps_done = accepted.astype(jnp.float32)[:, None]
    index = jnp.arange(props, dtype=jnp.float32)[None, :]
    age = jnp.maximum(steps_done - 1.0 - index, 0.0)
    weights = jnp.where(
        (index < steps_done)[:, :, None], jnp.exp(-decays[None, None, :] * age[:, :, None]), 0.0
    )
    kept = jnp.exp(-decays[None, :] * steps_done)
    added = jnp.einsum("bphd,bphe->bhde", old_keys * weights[..., None], old_values, precision=HIGH)
    return kept[:, :, None, None] * state + added


def retain(queries, key_rows, val_rows, gate_rows, decays, carried, parents, accepted, seq_length):
    nseq, props, heads, head_dim = queries.shape
    ancestry, depths = ancestry_of(parents)
    positions = (seq_length + accepted).astype(jnp.float32)[:, None] + depths
    rotated_q = rotate(queries.astype(jnp.float32), positions)
    rotated_k = rotate(key_rows.astype(jnp.float32), positions) * head_dim ** (-0.5)
    scores = jnp.einsum("bihd,bjhd->bhij", rotated_q, rotated_k, precision=HIGH)
    spacing = jnp.maximum(depths[:, :, None] - depths[:, None, :], 0.0)
    weighting = ancestry[:, None] * jnp.exp(-decays[None, :, None, None] * spacing[:, None])
    within = jnp.einsum(
        "bhij,bjhe->bihe", scores * weighting, val_rows.astype(jnp.float32), precision=HIGH
    )
    state_scale = jnp.exp(-decays[None, None, :] * (depths[:, :, None] + 1.0))
    from_state = (
        jnp.einsum("bihd,bhde->bihe", rotated_q, carried, precision=HIGH) * state_scale[..., None]
    )
    mixed_raw = within + from_state
    average = jnp.mean(mixed_raw, axis=-1, keepdims=True)
    centred = mixed_raw - average
    variance = jnp.mean(centred * centred, axis=-1, keepdims=True)
    normed = (centred * lax.rsqrt(variance + EPS)).reshape(nseq * props, heads * head_dim)
    gates = gate_rows.astype(jnp.float32).reshape(nseq * props, heads * head_dim)
    return (normed * jax.nn.silu(gates)).astype(jnp.bfloat16)


def per_device(
    tokens,
    norm_gain,
    w_query,
    w_key,
    w_value,
    w_gate,
    w_output,
    decay_rate,
    state,
    prev_keys,
    prev_values,
    accepted,
    parents,
    seq_length,
):
    weights = jnp.concatenate([w_query, w_key, w_value, w_gate], axis=1)
    columns = weights.shape[1]
    whole = lax.all_gather(tokens, ("kv", "tp"), axis=1, tiled=True).astype(jnp.float32)
    scale = lax.rsqrt(jnp.mean(whole * whole, axis=1, keepdims=True) + EPS)
    full_normed = (whole * scale * norm_gain[None, :]).astype(jnp.bfloat16)
    projected = jnp.dot(full_normed, weights, preferred_element_type=jnp.float32)
    rows_count = tokens.shape[0]
    projected = projected.astype(jnp.bfloat16).reshape(rows_count, 4, columns // 4)
    regrouped = lax.all_to_all(projected, ("kv", "tp"), split_axis=0, concat_axis=2, tiled=True)
    nseq = state.shape[0]
    heads = decay_rate.shape[0]
    head_dim = state.shape[2]
    props = parents.shape[1]

    def shaped(role):
        return regrouped[:, role].reshape(nseq, props, heads, head_dim)

    carried = advance(state, prev_keys, prev_values, accepted, decay_rate)
    mixed = retain(
        shaped(0),
        shaped(1),
        shaped(2),
        shaped(3),
        decay_rate,
        carried,
        parents,
        accepted,
        seq_length,
    )
    output = jnp.dot(
        lax.all_gather(mixed, ("kv", "tp"), axis=0, tiled=True),
        w_output,
        preferred_element_type=jnp.float32,
    ).astype(jnp.bfloat16)
    return (output, carried)


MESH = pl.DeviceIdType.MESH


def cos_sin(angles):
    quarter = jnp.floor(angles * (2.0 / np.pi) + 0.5)
    rest = angles - quarter * 1.5703125
    rest = rest - quarter * 4.8375129699707031e-4
    rest = rest - quarter * 7.549789948768648e-8
    sq = rest * rest
    sine = rest + rest * sq * (-1.6666654611e-1 + sq * (8.3321608736e-3 - sq * 1.9515295891e-4))
    cosine = 1.0 - 0.5 * sq + sq * sq * (
        4.166664568298827e-2 + sq * (-1.388731625493765e-3 + sq * 2.443315711809948e-5)
    )
    which = quarter.astype(jnp.int32)
    swap = (which & 1) == 1
    sin_out = jnp.where(swap, cosine, sine)
    cos_out = jnp.where(swap, sine, cosine)
    sin_out = jnp.where((which & 2) == 2, -sin_out, sin_out)
    cos_out = jnp.where(((which + 1) & 2) == 2, -cos_out, cos_out)
    return cos_out, sin_out


def swap_rows(x):
    return pltpu.roll(x, 4, axis=x.ndim - 2)


def fused(
    kv_size,
    heads,
    decay_hbm,
    accepted_hbm,
    parents_hbm,
    length_hbm,
    tokens_hbm,
    gain_hbm,
    freq_hbm,
    wq_hbm,
    wk_hbm,
    wv_hbm,
    wg_hbm,
    wo_hbm,
    state_hbm,
    pk_hbm,
    pv_hbm,
    mg,
    carried,
    w_out,
    xg,
    gain,
    freq,
    w_all,
    state,
    pk,
    pv,
    split,
    dtab,
    stab,
    stage,
    recvq,
    decay_ref,
    accepted_ref,
    parents_ref,
    length_ref,
    local_sem,
    w_sem,
    x_send,
    x_recv,
    p_send,
    p_recv,
    m_send,
    m_recv,
):
    n = kv_size * 2
    kv, tp = lax.axis_index("kv"), lax.axis_index("tp")
    me = kv * 2 + tp
    block = xg.shape[2]
    cols = wq_hbm.shape[1]
    per = cols // 128

    ranked = [sorted(range(kv_size), key=lambda o: abs(o - z)) for z in range(kv_size)]
    seat = [
        sum(jnp.where(kv == z, ranked[z][d], 0) for z in range(kv_size)) for d in range(kv_size)
    ]

    def owner(d, dt):
        return seat[d] * 2 + (1 - tp if dt else tp)

    def target(d, dt):
        return {"kv": seat[d], "tp": 1 - tp if dt else tp}

    near = list(range(1, kv_size))
    far = near[::-1]
    order = [(0, 0), (0, 1)] + [(d, 0) for d in near] + [(d, 1) for d in near]

    def local(src, dst, i):
        return pltpu.make_async_copy(src, dst, local_sem.at[i])

    barrier = pltpu.get_barrier_semaphore()
    for dz in range(kv_size):
        for dt in range(2):
            if dz or dt:
                pl.semaphore_signal(barrier, inc=1, device_id=target(dz, dt), device_id_type=MESH)
    tok_copy = local(tokens_hbm, xg.at[me], 0)
    tok_copy.start()
    scalars = [
        local(decay_hbm, decay_ref, 7),
        local(accepted_hbm, accepted_ref, 8),
        local(parents_hbm, parents_ref, 9),
        local(length_hbm, length_ref, 10),
    ]
    for c in scalars:
        c.start()
    small = [
        local(gain_hbm, gain, 1),
        local(freq_hbm, freq, 2),
        local(pk_hbm, pk, 3),
        local(pv_hbm, pv, 4),
    ]
    for c in small:
        c.start()
    small.append(local(state_hbm, state, 5))
    w_copies = []
    for t, (dz, dt) in enumerate(order):
        rows = pl.ds(pl.multiple_of(owner(dz, dt) * block, block), block)
        these = []
        for r, ref in enumerate((wq_hbm, wk_hbm, wv_hbm, wg_hbm)):
            c = pltpu.make_async_copy(
                ref.at[rows], w_all.at[rows, pl.ds(r * cols, cols)], w_sem.at[t, r]
            )
            these.append(c)
        w_copies.append(these)
    wo_copy = local(wo_hbm, w_out, 6)

    def load(t):
        for c in w_copies[t]:
            c.start()


    def gather_start(buf, send_sem, recv_sem):
        sends = {}
        for dz in far:
            sends[dz, 0] = pltpu.make_async_remote_copy(
                src_ref=buf.at[me], dst_ref=buf.at[me], send_sem=send_sem.at[dz],
                recv_sem=recv_sem.at[kv], device_id=target(dz, 0), device_id_type=MESH,
            )
        sends[0, 1] = pltpu.make_async_remote_copy(
            src_ref=buf.at[me], dst_ref=buf.at[me], send_sem=send_sem.at[kv_size],
            recv_sem=recv_sem.at[kv_size + kv], device_id=target(0, 1), device_id_type=MESH,
        )
        for c in sends.values():
            c.start()
        return sends

    def relay(buf, send_sem, recv_sem, dz):
        slot = buf.at[owner(dz, 0)]
        c = pltpu.make_async_remote_copy(
            src_ref=slot, dst_ref=slot, send_sem=send_sem.at[kv_size + dz],
            recv_sem=recv_sem.at[kv_size + seat[dz]], device_id=target(0, 1), device_id_type=MESH,
        )
        c.start()
        return c

    def arrived(buf, send_sem, recv_sem, dz, dt):
        slot = buf.at[owner(dz, dt)]
        i = seat[dz] + dt * kv_size
        pltpu.make_async_remote_copy(
            src_ref=slot, dst_ref=slot, send_sem=send_sem.at[i], recv_sem=recv_sem.at[i],
            device_id=target(0, 1), device_id_type=MESH,
        ).wait_recv()

    tok_copy.wait()
    for t in range(2):
        load(t)
    pl.semaphore_wait(barrier, n - 1)
    x_sends = gather_start(xg, x_send, x_recv)
    for t in range(2, n):
        load(t)
    small[-1].start()

    for c in scalars:
        c.wait()
    row = lax.broadcasted_iota(jnp.int32, (8, 128), 0)
    lane = lax.broadcasted_iota(jnp.int32, (8, 128), 1)
    which = row & 3
    low = row < 4
    props = 4
    parent = [parents_ref[0, i] for i in range(props)]
    anc = [[jnp.int32(1 if i == j else 0) for j in range(props)] for i in range(props)]
    depth = [jnp.int32(0) for i in range(props)]
    for i in range(1, props):
        for j in range(i):
            hit = jnp.where(parent[i] == j, jnp.int32(1), jnp.int32(0))
            depth[i] = depth[i] + hit * (depth[j] + 1)
            for m in range(i):
                anc[i][m] = anc[i][m] + hit * anc[j][m]

    def by_row(values):
        out = jnp.full((8, 128), values[0], jnp.int32)
        for i in range(1, props):
            out = jnp.where(which == i, jnp.full((8, 128), values[i], jnp.int32), out)
        return out.astype(jnp.float32)

    deep = by_row(depth)
    acc_count = jnp.full((8, 128), accepted_ref[0, 0], jnp.int32).astype(jnp.float32)
    base = jnp.full((8, 128), accepted_ref[0, 0] + length_ref[0, 0], jnp.int32).astype(jnp.float32)
    index = which.astype(jnp.float32)
    age = jnp.maximum(acc_count - 1.0 - index, 0.0)
    live = jnp.where(index < acc_count, 1.0, 0.0)
    spacing = [jnp.maximum(deep - depth[j].astype(jnp.float32), 0.0) for j in range(props)]
    kin = [jnp.where(low, by_row([anc[i][j] for i in range(props)]), 0.0) for j in range(props)]

    for c in small[:-1]:
        c.wait()
    cosine, sine = cos_sin((base + deep) * freq[...])
    row_scale = jnp.where(low, 1.0, 128.0 ** -0.5)
    cos_t = cosine * row_scale
    sin_t = jnp.where(lane < 64, -sine, sine) * row_scale

    squares = jnp.zeros((xg.shape[1], 128), jnp.float32)
    total = None

    def project(total, squares, t, dz, dt):
        who = owner(dz, dt)
        for c in w_copies[t]:
            c.wait()
        x = xg[who].astype(jnp.float32)
        for q in range(block // 128):
            part = x[:, q * 128:(q + 1) * 128]
            squares = squares + part * part
        at = pl.ds(pl.multiple_of(who * block, block), block)
        xn = (x * gain[:, at]).astype(jnp.bfloat16)
        y = jnp.dot(xn, w_all[at, :], preferred_element_type=jnp.float32)
        return (y if total is None else total + y), squares

    total, squares = project(total, squares, 0, 0, 0)
    arrived(xg, x_send, x_recv, 0, 1)
    total, squares = project(total, squares, 1, 0, 1)
    relays = []
    waited = set()
    for t, (dz, dt) in enumerate(order):
        if t < 2:
            continue
        if dt == 0:
            for d in (near[:2] if dz in near[:2] else [dz]):
                if d not in waited:
                    waited.add(d)
                    arrived(xg, x_send, x_recv, d, 0)
                    relays.append(relay(xg, x_send, x_recv, d))
        else:
            arrived(xg, x_send, x_recv, dz, 1)
        total, squares = project(total, squares, t, dz, dt)
    width = block * n
    scale = lax.rsqrt(jnp.sum(squares, axis=1, keepdims=True) * (1.0 / width) + EPS)
    total = total * scale
    low_c = lax.broadcasted_iota(jnp.int32, (8, cols), 0) < 4
    for t in range(n // 2):
        q, k, v, g = [total[8 * t:8 * t + 8, r * cols:(r + 1) * cols] for r in range(4)]
        stage[2 * t] = jnp.concatenate(
            [jnp.where(low_c, q, swap_rows(k)), jnp.where(low_c, v, swap_rows(g))], axis=0
        ).astype(jnp.bfloat16)
        stage[2 * t + 1] = jnp.concatenate(
            [jnp.where(low_c, swap_rows(q), k), jnp.where(low_c, swap_rows(v), g)], axis=0
        ).astype(jnp.bfloat16)
    p_sends = []
    for dz in far + [0]:
        for dt in range(2):
            if dz or dt:
                to = target(dz, dt)
                c = pltpu.make_async_remote_copy(
                    src_ref=stage.at[to["kv"] * 2 + to["tp"]], dst_ref=recvq.at[me],
                    send_sem=p_send.at[dz * 2 + dt], recv_sem=p_recv.at[me],
                    device_id=to, device_id_type=MESH,
                )
                c.start()
                p_sends.append(c)
    wo_copy.start()
    recvq[me] = stage[me]
    small[-1].wait()

    def advance_head(h, carry):
        rate = jnp.full((8, 128), decay_ref[h], jnp.float32)
        for j in range(props):
            dtab[h, j] = kin[j] * jnp.exp(-rate * spacing[j])
        stab[h] = jnp.exp(-rate * (deep + 1.0))
        at = pl.ds(pl.multiple_of(h * 128, 128), 128)
        kh = pk[0, :, at].astype(jnp.float32)
        vh = pv[0, :, at].astype(jnp.float32)
        weighted = jnp.concatenate([kh, kh], axis=0) * (live * jnp.exp(-rate * age))
        upper = weighted.astype(jnp.bfloat16).astype(jnp.float32)
        both = jnp.where(low, upper, weighted - upper)
        v2 = jnp.concatenate([vh, vh], axis=0).astype(jnp.bfloat16)
        added = lax.dot_general(
            both.T.astype(jnp.bfloat16), v2, (((1,), (0,)), ((), ())),
            preferred_element_type=jnp.float32,
        )
        kept = jnp.exp(-rate * acc_count)[0:1]
        new = kept * state[0, h] + added
        carried[0, h] = new
        big = new.astype(jnp.bfloat16)
        split[h, :, 0:128] = big
        split[h, :, 128:256] = (new - big.astype(jnp.float32)).astype(jnp.bfloat16)
        return carry

    lax.fori_loop(0, heads, advance_head, 0, unroll=2)

    for dz in range(kv_size):
        for dt in range(2):
            if dz or dt:
                slot = recvq.at[owner(dz, dt)]
                i = owner(dz, dt)
                pltpu.make_async_remote_copy(
                    src_ref=slot, dst_ref=slot, send_sem=p_send.at[i], recv_sem=p_recv.at[i],
                    device_id=target(0, 1), device_id_type=MESH,
                ).wait_recv()

    low3 = low[None]
    for k in range(per):
        got = recvq[:, :, k * 128:(k + 1) * 128].astype(jnp.float32)
        qk, vg = got[:, 0:8], got[:, 8:16]
        turned = qk * cos_t[None] + pltpu.roll(qk, 64, axis=2) * sin_t[None]
        mine = [dtab[s * per + k] for s in range(n)]
        decay = jnp.stack([stab[s * per + k] for s in range(n)])
        qs = turned * decay
        qs = jnp.where(low3, qs, swap_rows(qs))
        upper = qs.astype(jnp.bfloat16).astype(jnp.float32)
        pair = jnp.where(low3, upper, qs - upper).astype(jnp.bfloat16)
        raws = []
        for s in range(n):
            y = jnp.dot(pair[s], split[s * per + k], preferred_element_type=jnp.float32)
            raws.append(y[:, 0:128] + y[:, 128:256])
        raw = jnp.stack(raws)
        raw = raw + swap_rows(raw)
        for j in range(props):
            score = jnp.sum(turned * turned[:, 4 + j:5 + j, :], axis=2, keepdims=True)
            raw = raw + score * jnp.stack([m[j] for m in mine]) * vg[:, j:j + 1, :]
        centred = raw - jnp.sum(raw, axis=2, keepdims=True) * (1.0 / 128)
        spread = jnp.sum(centred * centred, axis=2, keepdims=True) * (1.0 / 128)
        gate = swap_rows(vg)
        mixed = centred * lax.rsqrt(spread + EPS) * (gate / (1.0 + jnp.exp(-gate)))
        group = n // 4
        for b in range(group):
            first = jnp.where(low, mixed[b], swap_rows(mixed[group + b]))
            second = jnp.where(low, mixed[2 * group + b], swap_rows(mixed[3 * group + b]))
            at = b * cols + k * 128
            mg[me, :, at:at + 128] = jnp.concatenate([first, second], axis=0).astype(jnp.bfloat16)

    m_sends = gather_start(mg, m_send, m_recv)
    m_relays = []
    for dz in near:
        arrived(mg, m_send, m_recv, dz, 0)
        m_relays.append(relay(mg, m_send, m_recv, dz))
    arrived(mg, m_send, m_recv, 0, 1)
    for dz in near:
        arrived(mg, m_send, m_recv, dz, 1)
    wo_copy.wait()
    for c in list(x_sends.values()) + relays + p_sends + list(m_sends.values()) + m_relays:
        c.wait_send()


def finish(mg, carried, w_out, out_hbm, carried_hbm, lhs, outb, sem):
    heads = carried.shape[1]
    pieces = 8 if heads % 8 == 0 else 1
    count = heads // pieces
    carried_copies = []
    for i in range(pieces):
        at = pl.ds(i * count, count)
        c = pltpu.make_async_copy(carried.at[:, at], carried_hbm.at[:, at], sem.at[i])
        c.start()
        carried_copies.append(c)
    chunk = mg.shape[2]
    low_m = lax.broadcasted_iota(jnp.int32, (8, chunk), 0) < 4
    for t in range(mg.shape[0] // 2):
        one = mg[2 * t].astype(jnp.float32)
        two = mg[2 * t + 1].astype(jnp.float32)
        for c in range(4):
            at = 8 * (c // 2)
            a, b = one[at:at + 8], two[at:at + 8]
            if c % 2 == 0:
                piece = jnp.where(low_m, a, swap_rows(b))
            else:
                piece = jnp.where(low_m, swap_rows(a), b)
            lhs[8 * t:8 * t + 8, c * chunk:(c + 1) * chunk] = piece
    outb[...] = jnp.dot(
        lhs[...].astype(jnp.bfloat16), w_out[...], preferred_element_type=jnp.float32
    ).astype(jnp.bfloat16)
    out_copy = pltpu.make_async_copy(outb, out_hbm, sem.at[8])
    out_copy.start()
    out_copy.wait()
    for c in carried_copies:
        c.wait()


def fused_device(
    kv_size, tokens, norm_gain, w_query, w_key, w_value, w_gate, w_output, decay_rate, state,
    prev_keys, prev_values, accepted, parents, seq_length,
):
    n = kv_size * 2
    rows, block = tokens.shape
    width, cols = w_query.shape
    heads = decay_rate.shape[0]
    hid, out_cols = w_output.shape
    freq = 10000.0 ** (-(np.arange(128) % 64) / 64.0)
    freq = jnp.asarray(freq.astype(np.float32)[None, :])
    hbm = pl.BlockSpec(memory_space=pltpu.HBM)
    vmem = pl.BlockSpec(memory_space=pltpu.VMEM)
    bf, f32 = jnp.bfloat16, jnp.float32
    dma = pltpu.SemaphoreType.DMA
    room = 67043328 - state.size * 4 - hid * out_cols * 2 - n * 16 * (hid // 4) * 2
    gathered, new_state, w_near = pl.pallas_call(
        functools.partial(fused, kv_size, heads),
        out_shape=(
            pltpu.VMEM((n, 16, hid // 4), bf),
            pltpu.VMEM(state.shape, f32),
            pltpu.VMEM((hid, out_cols), bf),
        ),
        in_specs=[hbm] * 15,
        out_specs=(vmem, vmem, vmem),
        scratch_shapes=[
            pltpu.VMEM((n, rows, block), bf),
            pltpu.VMEM((1, width), f32),
            pltpu.VMEM((1, 128), f32),
            pltpu.VMEM((width, 4 * cols), bf),
            pltpu.VMEM(state.shape, f32),
            pltpu.VMEM(prev_keys.shape, bf),
            pltpu.VMEM(prev_values.shape, bf),
            pltpu.VMEM((heads, 128, 256), bf),
            pltpu.VMEM((heads, 4, 8, 128), f32),
            pltpu.VMEM((heads, 8, 128), f32),
            pltpu.VMEM((n, 16, cols), bf),
            pltpu.VMEM((n, 16, cols), bf),
            pltpu.SMEM(decay_rate.shape, f32),
            pltpu.SMEM((1, 1), jnp.int32),
            pltpu.SMEM(parents.shape, jnp.int32),
            pltpu.SMEM((1, 1), jnp.int32),
            dma((11,)),
            dma((n, 4)),
            dma((n,)),
            dma((n,)),
            dma((n,)),
            dma((n,)),
            dma((n,)),
            dma((n,)),
        ],
        compiler_params=pltpu.CompilerParams(
            collective_id=0, has_side_effects=True, vmem_limit_bytes=room
        ),
    )(
        decay_rate, accepted[None, :], parents, seq_length[None, :], tokens, norm_gain[None, :], freq, w_query,
        w_key, w_value, w_gate, w_output, state, prev_keys, prev_values,
    )
    return pl.pallas_call(
        finish,
        out_shape=(
            jax.ShapeDtypeStruct((rows, out_cols), bf),
            jax.ShapeDtypeStruct(state.shape, f32),
        ),
        in_specs=[vmem] * 3,
        out_specs=(hbm, hbm),
        scratch_shapes=[
            pltpu.VMEM((rows, hid), f32),
            pltpu.VMEM((rows, out_cols), bf),
            dma((9,)),
        ],
        compiler_params=pltpu.CompilerParams(vmem_limit_bytes=8 * 1024 * 1024),
    )(gathered, new_state, w_near)


def choose(kv_size, tp_size, *args):
    tokens, w_query, state, parents = args[0], args[2], args[8], args[12]
    n = kv_size * tp_size
    fits = (
        tp_size == 2
        and n % 4 == 0
        and kv_size > 2
        and state.shape[0] == 1
        and state.shape[2:] == (128, 128)
        and parents.shape[1] == 4
        and w_query.shape[1] % 128 == 0
        and tokens.shape[0] == 4 * n
        and tokens.shape[1] % 128 == 0
    )
    if fits:
        return fused_device(kv_size, *args)
    return per_device(*args)


def solution(mesh):
    placed = (
        P("dp", ("kv", "tp")),
        P(),
        P(None, ("kv", "tp")),
        P(None, ("kv", "tp")),
        P(None, ("kv", "tp")),
        P(None, ("kv", "tp")),
        P(None, ("kv", "tp")),
        P(),
        P(("dp", "kv", "tp"), None, None, None),
        P(("dp", "kv", "tp"), None, None),
        P(("dp", "kv", "tp"), None, None),
        P(("dp", "kv", "tp")),
        P(("dp", "kv", "tp"), None),
        P(("dp", "kv", "tp")),
    )
    return jax.shard_map(
        functools.partial(choose, mesh.shape["kv"], mesh.shape["tp"]),
        mesh=mesh,
        in_specs=placed,
        out_specs=(P("dp", ("kv", "tp")), P(("dp", "kv", "tp"), None, None, None)),
        check_vma=False,
    )
```
